32 devices in a mesh: gr: 2 (over x), fs: 8 (over z, y), tp: 2 (over core).
Axes of the slice: x: 2, y: 2, z: 4, core: 2. Of those that a mesh axis runs over, the one named last changes fastest.
Arguments:
- tokens: bfloat16 [16384, 3072], P(('gr', 'fs')), may hold values from -6 to 6
- norm_gain: float32 [3072], P(('gr', 'fs')), may hold values from 0.1 to 1.9
- gate_weight: float32 [8, 3072, 768], P(None, ('gr', 'fs'), 'tp'), may hold values from -0.109375 to 0.109375
- up_weight: float32 [8, 3072, 768], P(None, ('gr', 'fs'), 'tp'), may hold values from -0.109375 to 0.109375
- down_weight: float32 [8, 3072, 768], P(None, ('gr', 'fs'), 'tp'), may hold values from -0.21875 to 0.21875
- group_pick: int32 [16384], P(('gr', 'fs')), may hold values from 0 to 3, as said below
- expert_pick: int32 [16384, 2], P(('gr', 'fs')), may hold values from 0 to 1, as said below
- route_weight: float32 [16384, 2], P(('gr', 'fs')), may hold values from 0.1 to 1
Outputs:
- combined: bfloat16 [16384, 3072], P(('gr', 'fs'), 'tp')
- gate_served: bfloat16 [8, 3072, 768], P('fs', None, 'tp')
- up_served: bfloat16 [8, 3072, 768], P('fs', None, 'tp')
- down_served: bfloat16 [8, 3072, 768], P('fs', None, 'tp')
The draws below stay inside these ranges and needn't reach their ends.
Inputs may be any that keep to these rules, and one draw needn't show every extreme that they name: `group_pick`: in each aligned block of 1024 rows every group is picked by the same number of rows. `expert_pick`: the 2 entries of a row differ. In each aligned block of 1024 rows, every expert (group and number together) is named exactly 256 times.
All inputs are finite; a program needn't handle non-finite values.
Results may differ from the reference program's by a relative error of at most 0.0092.
Values may be sent and summed in bfloat16 or wider, within the bound.
No kernel may reach another device: no remote copies, remote signals or barrier semaphores. Data moves between devices by JAX's collectives and lax.ppermute only.
A program may use at most 128 MiB of HBM per device.

```python
import math
import jax
import jax.numpy as jnp
from jax import lax

D = 3072
FF = 768
GROUPS = 4
TOP = 2
TOK_DEV = 1024
EXPERTS = 8
TOKENS = 16384
N_TP = 2


def routing(key):
    blocks = TOKENS // TOK_DEV
    per_group = EXPERTS // GROUPS
    position = jnp.arange(TOK_DEV, dtype=jnp.int32)
    group_of = position % GROUPS
    within = position // GROUPS
    first_pick = within % per_group
    second_pick = (first_pick + 1 + within // per_group % (per_group - 1)) % per_group

    def one_block(block_key):
        order_key, label_key = jax.random.split(block_key)
        order = jax.random.permutation(order_key, TOK_DEV)
        relabel = jax.vmap(lambda label_one: jax.random.permutation(label_one, per_group))(jax.random.split(label_key, GROUPS))
        first_label = relabel[group_of, first_pick]
        second_label = relabel[group_of, second_pick]
        pairs = jnp.stack([first_label, second_label], axis=1).astype(jnp.int32)
        group_tok = jnp.zeros((TOK_DEV,), jnp.int32).at[order].set(group_of)
        pair_tok = jnp.zeros((TOK_DEV, 2), jnp.int32).at[order].set(pairs)
        return (group_tok, pair_tok)
    block_keys = jax.random.split(jax.random.fold_in(key, 71), blocks)
    groups_all, pairs_all = jax.vmap(one_block)(block_keys)
    return (groups_all.reshape(TOKENS).astype(jnp.int32), pairs_all.reshape(TOKENS, 2).astype(jnp.int32))


def draw_group_pick(key, part):
    return routing(key)[0]


def draw_expert_pick(key, part):
    return routing(key)[1]


def block_levels(own_key, dims, pieces, low, high):
    def one(dim, shards_of):
        heights = jax.random.uniform(jax.random.fold_in(jax.random.fold_in(own_key, 6), dim), (shards_of,), jnp.float32, low / len(pieces), high / len(pieces))
        return jnp.repeat(jnp.exp(heights), dims[dim] // shards_of).reshape((-1,) + (1,) * (len(dims) - dim - 1))

    loudness = one(*pieces[0])
    for cut in pieces[1:]:
        loudness = loudness * one(*cut)
    return loudness


def centred(own_key, extent, spread, bound, pieces=(), held_as=jnp.bfloat16):
    result = jax.random.normal(own_key, extent, jnp.float32) * spread
    if len(pieces) > 0:
        result = block_levels(own_key, extent, pieces, -0.22, 0.18) * result
    return jnp.clip(result, min=-bound, max=bound).astype(held_as)


def setup_inputs(seed: int = 0) -> dict:
    key_of = jax.random.split(jax.random.key(seed), 9)
    return {
        "tokens": centred(key_of[0], (TOKENS, D), 1.0, 6.0, ((0, 16),)),
        "norm_gain": jnp.clip(1.0 + 0.18 * jax.random.normal(key_of[1], (D,), jnp.float32), 0.1, 1.9),
        "gate_weight": centred(key_of[2], (EXPERTS, D, FF), D ** -0.5, 0.109375, ((1, 16), (2, 2)), jnp.float32),
        "up_weight": centred(key_of[3], (EXPERTS, D, FF), D ** -0.5, 0.109375, ((1, 16), (2, 2)), jnp.float32),
        "down_weight": centred(key_of[4], (EXPERTS, D, FF), FF ** -0.5, 0.21875, ((1, 16), (2, 2)), jnp.float32),
        "group_pick": draw_group_pick(jax.random.fold_in(key_of[8], 71), 0),
        "expert_pick": draw_expert_pick(jax.random.fold_in(key_of[8], 71), 0),
        "route_weight": jnp.clip(jnp.exp(math.log(1.0) - 2.3025851 * jax.random.uniform(key_of[7], (TOKENS, TOP), jnp.float32) ** block_levels(key_of[7], (TOKENS, TOP), ((0, 16),), -0.2, 0.2)), 0.1, 1.0),
    }


EPS = 1e-06

def reference(tokens, norm_gain, gate_weight, up_weight, down_weight, group_pick, expert_pick, route_weight):
    gate_served = (norm_gain[None, :, None] * gate_weight).astype(jnp.bfloat16)
    up_served = (norm_gain[None, :, None] * up_weight).astype(jnp.bfloat16)
    down_served = down_weight.astype(jnp.bfloat16)
    as_float = tokens.astype(jnp.float32)
    normed = (as_float * lax.rsqrt(lax.optimization_barrier(jnp.mean(as_float * as_float, axis=-1, keepdims=True)) + EPS)).astype(jnp.bfloat16)
    expert_ids = (group_pick[:, None] * (EXPERTS // GROUPS) + expert_pick).reshape(-1).astype(jnp.int32)
    per_expert = TOP * TOKENS // EXPERTS
    half_width = FF // N_TP

    def run_expert(expert_item):
        w_gate, w_up, w_down, index = expert_item
        row_ids = jnp.nonzero(expert_ids == index, size=per_expert)[0]
        rows_in = normed[row_ids // TOP]
        gate_acts = jnp.dot(rows_in, w_gate, preferred_element_type=jnp.float32)
        up_acts = jnp.dot(rows_in, w_up, preferred_element_type=jnp.float32)
        hidden = (jax.nn.silu(gate_acts) * up_acts).astype(jnp.bfloat16)
        accum_sum = jnp.zeros((per_expert, D), jnp.float32)
        for block in range(N_TP):
            part_sum = lax.dot_general(hidden[:, block * half_width:(block + 1) * half_width], w_down[:, block * half_width:(block + 1) * half_width], (((1,), (1,)), ((), ())), preferred_element_type=jnp.float32)
            accum_sum = accum_sum + lax.optimization_barrier(part_sum.astype(jnp.bfloat16)).astype(jnp.float32)
        return (accum_sum.astype(jnp.bfloat16), row_ids)
    outputs, row_ids = lax.map(run_expert, (gate_served, up_served, down_served, jnp.arange(EXPERTS, dtype=jnp.int32)))
    flat_out = jnp.zeros((TOP * TOKENS, D), jnp.bfloat16).at[row_ids.reshape(-1)].set(outputs.reshape(-1, D))
    combined = lax.optimization_barrier(jnp.sum(route_weight[:, :, None] * flat_out.reshape(TOKENS, TOP, D).astype(jnp.float32), axis=1))
    return (combined.astype(jnp.bfloat16), gate_served, up_served, down_served)
```

```python
import functools

import jax
import jax.numpy as jnp
from jax import lax
from jax.experimental import pallas as pl
from jax.experimental.pallas import tpu as pltpu
from jax.sharding import PartitionSpec as P

GROUPS = 4


EPS = 1e-06

CHUNKS = 2


def general(
    tokens, norm_gain, gate_weight, up_weight, down_weight, group_pick, expert_pick, route_weight
):
    scaled = norm_gain[None, :, None]
    gate_local = (scaled * gate_weight).astype(jnp.bfloat16)
    up_local = (scaled * up_weight).astype(jnp.bfloat16)
    down_local = down_weight.astype(jnp.bfloat16)
    experts, _, cols_dev = gate_local.shape

    def served(mine):
        half = lax.all_to_all(mine, "fs", split_axis=0, concat_axis=1, tiled=True)
        return lax.all_gather(half, "gr", axis=1, tiled=True).reshape(1, -1, cols_dev)

    gate_new = served(gate_local)
    up_new = served(up_local)
    down_new = served(down_local)
    tok_rows, model_width = tokens.shape
    as_float = tokens.astype(jnp.float32)
    normed = (
        as_float * lax.rsqrt(jnp.mean(as_float * as_float, axis=-1, keepdims=True) + EPS)
    ).astype(jnp.bfloat16)
    per_group = experts // GROUPS
    top_count = expert_pick.shape[1]
    capacity = top_count * tok_rows // experts
    flat_ids = (group_pick[:, None] * per_group + expert_pick).reshape(-1)
    onehot = (flat_ids[:, None] == jnp.arange(experts, dtype=jnp.int32)[None, :]).astype(jnp.int32)
    slot_index = jnp.sum(onehot * (jnp.cumsum(onehot, axis=0) - 1), axis=1)
    target = flat_ids * capacity + slot_index
    source = (
        jnp.zeros((experts * capacity,), jnp.int32)
        .at[target]
        .set(jnp.arange(top_count * tok_rows, dtype=jnp.int32) // top_count)
    )
    outgoing = normed[source].reshape(experts, capacity, model_width)
    share = capacity // lax.axis_size("tp")
    start = lax.axis_index("tp") * share
    my_share = lax.dynamic_slice_in_dim(outgoing, start, share, 1)
    landed = lax.all_to_all(my_share, "fs", split_axis=0, concat_axis=1, tiled=True).reshape(
        experts, share, model_width
    )
    arrived = lax.all_gather(landed, "tp", axis=1, tiled=True).reshape(-1, model_width)
    gate_acts = jnp.dot(arrived, gate_new[0], preferred_element_type=jnp.float32)
    up_acts = jnp.dot(arrived, up_new[0], preferred_element_type=jnp.float32)
    hidden = (jax.nn.silu(gate_acts) * up_acts).astype(jnp.bfloat16)
    partial_value = lax.dot_general(
        hidden, down_new[0], (((1,), (1,)), ((), ())), preferred_element_type=jnp.float32
    ).astype(jnp.bfloat16)
    summed = (
        lax.psum_scatter(partial_value, "tp", scatter_dimension=1, tiled=True)
        .astype(jnp.float32)
        .astype(jnp.bfloat16)
    )
    returned = lax.all_to_all(summed, "fs", split_axis=0, concat_axis=0, tiled=True)
    picked = returned[target].reshape(tok_rows, top_count, -1).astype(jnp.float32)
    combined = jnp.sum(route_weight[:, :, None] * picked, axis=1).astype(jnp.bfloat16)
    return (combined, gate_new, up_new, down_new)


def assemble_body(place_ref, line_ref, across_ref, beside_ref, diag_a_ref, diag_b_ref, own_ref, other_ref):
    row, group, member = place_ref[0], place_ref[1], place_ref[2]
    blocks = line_ref.shape[1]
    for k in range(blocks):
        near = group ^ k
        for which, out_ref in ((member, own_ref), (1 - member, other_ref)):
            out_ref[row, near, member] = line_ref[which, k]
            out_ref[1 - row, near, member] = across_ref[which, k]
            out_ref[row, near, 1 - member] = beside_ref[which, k]

        @pl.when(member == 0)
        def _():
            own_ref[1 - row, near, 1 - member] = diag_a_ref[k]
            other_ref[1 - row, near, 1 - member] = diag_b_ref[k]

        @pl.when(member == 1)
        def _():
            own_ref[1 - row, near, 1 - member] = diag_b_ref[k]
            other_ref[1 - row, near, 1 - member] = diag_a_ref[k]


def assemble(place, line, across, beside, diag_a, diag_b):
    members, blocks, rows_dev, cols = line.shape
    shape = jax.ShapeDtypeStruct((2, blocks, members, rows_dev, cols), line.dtype)
    size = 2 * 2 * blocks * members * rows_dev * cols
    own, other = pl.pallas_call(
        assemble_body,
        out_shape=(shape, shape),
        in_specs=[pl.BlockSpec(memory_space=pltpu.SMEM)] + [pl.BlockSpec(memory_space=pltpu.VMEM)] * 5,
        out_specs=(pl.BlockSpec(memory_space=pltpu.VMEM),) * 2,
        cost_estimate=pl.CostEstimate(flops=4 * size, bytes_accessed=4 * size, transcendentals=0),
        compiler_params=pltpu.CompilerParams(vmem_limit_bytes=32 * 1024 * 1024),
    )(place, line, across, beside, diag_a, diag_b)
    return own.reshape(-1, cols), other.reshape(-1, cols)


def paired(
    tokens, norm_gain, gate_weight, up_weight, down_weight, group_pick, expert_pick, route_weight
):
    experts, rows_dev, cols_dev = gate_weight.shape
    members = experts // GROUPS
    fs_size = lax.axis_size("fs")
    fs = lax.axis_index("fs")
    row, core = lax.axis_index("gr"), lax.axis_index("tp")
    group, member = fs // members, fs % members
    place = jnp.stack([row, group, member]).astype(jnp.int32)

    def swap_x(value):
        return lax.ppermute(value, "gr", [(0, 1), (1, 0)])

    def swap_y(value):
        return lax.ppermute(value, "fs", [(i, i ^ 1) for i in range(fs_size)])

    def swap_core(value):
        return lax.ppermute(value, "tp", [(0, 1), (1, 0)])

    def to_group(value, k):
        return lax.ppermute(value, "fs", [(i, i ^ (k * members)) for i in range(fs_size)])

    scaled = norm_gain[None, :, None]

    def rounded(weight, k, scale):
        part = lax.dynamic_slice_in_dim(weight, (group ^ k) * members, members, 0)
        return (scale * part if scale is not None else part).astype(jnp.bfloat16)

    def served(weight, scale):
        blocks = [rounded(weight, k, scale) for k in range(GROUPS)]
        got = [blocks[0]] + [to_group(blocks[k], k) for k in range(1, GROUPS)]
        line = jnp.stack(got, axis=1)
        across, beside = swap_x(line), swap_y(line)
        diag_a, diag_b = swap_y(across[0]), swap_x(beside[1])
        return assemble(place, line, across, beside, diag_a, diag_b)

    gate_own, gate_other = served(gate_weight, scaled)
    up_own, up_other = served(up_weight, scaled)
    down_own, down_other = served(down_weight, None)

    tok_rows, model_width = tokens.shape
    capacity = tok_rows // GROUPS
    half = capacity // 2
    sub = half // CHUNKS
    in_group = group_pick[:, None] == jnp.arange(GROUPS, dtype=jnp.int32)[None, :]
    counts = in_group.astype(jnp.int32)
    rank = jnp.sum(counts * (jnp.cumsum(counts, axis=0) - 1), axis=1)
    near = group_pick ^ group
    side, chunk, step = rank // half, rank % half // sub, rank % sub
    send_key = jnp.where(side == core, (chunk * GROUPS + near) * sub + step, -1)
    slots = jnp.arange(tok_rows // 2, dtype=jnp.int32)
    gather = (slots[:, None] == send_key[None, :]).astype(jnp.bfloat16)
    sorted_rows = jnp.dot(gather, tokens, preferred_element_type=jnp.float32).astype(jnp.bfloat16)
    as_float = sorted_rows.astype(jnp.float32)
    normed = (
        as_float * lax.rsqrt(jnp.mean(as_float * as_float, axis=-1, keepdims=True) + EPS)
    ).astype(jnp.bfloat16)
    normed = normed.reshape(CHUNKS, GROUPS, sub, model_width)

    by_member = [
        jnp.sum(jnp.where(expert_pick == m, route_weight, 0.0), axis=1) for m in range(members)
    ]
    rank_key = near * capacity + rank
    ranks = jnp.arange(tok_rows, dtype=jnp.int32)
    at_slot = ranks[:, None] == rank_key[None, :]
    weights = jnp.stack(
        [jnp.sum(jnp.where(at_slot, w[None, :], 0.0), axis=1) for w in by_member]
    ).reshape(members, GROUPS, capacity)
    got_weights = [weights[:, 0]] + [to_group(weights[:, k], k) for k in range(1, GROUPS)]
    held = jnp.stack(got_weights, axis=1).reshape(members, GROUPS, 2, CHUNKS, sub)
    held = jnp.where(core == 0, held, held[:, :, ::-1])
    held = jnp.where(member == 0, held, held[::-1])

    width = model_width // 2
    mine = core * width

    def hidden_of(rows, gate, up):
        gate_acts = jnp.dot(rows, gate, preferred_element_type=jnp.float32)
        up_acts = jnp.dot(rows, up, preferred_element_type=jnp.float32)
        return (jax.nn.silu(gate_acts) * up_acts).astype(jnp.bfloat16)

    def project(hidden, down, start):
        part = lax.dynamic_slice_in_dim(down, start, width, 0)
        return lax.dot_general(
            hidden, part, (((1,), (1,)), ((), ())), preferred_element_type=jnp.float32
        ).astype(jnp.bfloat16)

    pieces = []
    for c in range(CHUNKS):
        got = [normed[c, 0]] + [to_group(normed[c, k], k) for k in range(1, GROUPS)]
        ours = jnp.concatenate(got, axis=0)
        theirs = swap_core(ours)
        rows = jnp.concatenate([ours, theirs], axis=0)
        kept, sent = [], []
        for gate, up, down in ((gate_own, up_own, down_own), (gate_other, up_other, down_other)):
            hidden = hidden_of(rows, gate, up)
            turned = jnp.concatenate([hidden[GROUPS * sub :], hidden[: GROUPS * sub]], axis=0)
            sent.append(project(turned, down, width - mine))
            kept.append(project(hidden, down, mine))
        total = jnp.zeros((2, GROUPS, sub, width), jnp.float32)
        for e in range(2):
            both = kept[e].astype(jnp.float32) + swap_core(sent[e]).astype(jnp.float32)
            out = both.astype(jnp.bfloat16).astype(jnp.float32).reshape(2, GROUPS, sub, width)
            scale = jnp.transpose(held[e, :, :, c], (1, 0, 2))
            total = total + scale[..., None] * out
        result = total.astype(jnp.bfloat16)
        for k in range(GROUPS):
            block = result[:, k].reshape(2 * sub, width)
            pieces.append(block if k == 0 else to_group(block, k))

    back_key = ((chunk * GROUPS + near) * 2 + (side ^ core)) * sub + step
    scatter = (back_key[:, None] == ranks[None, :]).astype(jnp.bfloat16)
    combined = jnp.dot(
        scatter, jnp.concatenate(pieces, axis=0), preferred_element_type=jnp.float32
    ).astype(jnp.bfloat16)
    return (combined, gate_own[None], up_own[None], down_own[None])


def local(*args):
    experts, top_count = args[2].shape[0], args[6].shape[1]
    members = experts // GROUPS
    fits = (
        members == top_count == 2
        and lax.axis_size("gr") == lax.axis_size("tp") == 2
        and lax.axis_size("fs") == experts
        and args[0].shape[0] % (GROUPS * 2 * CHUNKS * 16) == 0
        and args[0].shape[1] % 256 == 0
    )
    return paired(*args) if fits else general(*args)


def solution(mesh):
    in_specs = (
        P(("gr", "fs"), None),
        P(("gr", "fs")),
        P(None, ("gr", "fs"), "tp"),
        P(None, ("gr", "fs"), "tp"),
        P(None, ("gr", "fs"), "tp"),
        P(("gr", "fs")),
        P(("gr", "fs"), None),
        P(("gr", "fs"), None),
    )
    out_specs = (
        P(("gr", "fs"), "tp"),
        P("fs", None, "tp"),
        P("fs", None, "tp"),
        P("fs", None, "tp"),
    )
    return jax.shard_map(local, mesh=mesh, in_specs=in_specs, out_specs=out_specs, check_vma=False)
```
